32 devices in a mesh: gr: 2 (over x), sp: 8 (over z, y), tp: 2 (over core).
Axes of the slice: x: 2, y: 2, z: 4, core: 2. Of those that a mesh axis runs over, the one named last changes fastest.
Arguments:
- tokens: bfloat16 [2, 2, 6144, 2048], P('gr', 'tp', 'sp'), may hold values from -6 to 6
- key_weight: bfloat16 [2048, 2048], replicated, may hold values from -0.125 to 0.125
- value_weight: bfloat16 [2048, 2048], replicated, may hold values from -0.125 to 0.125
- cum_gate: float32 [2, 32, 2, 6144], P('gr', None, 'tp', 'sp'), may hold values from -12588 to 0, as said below
- query: bfloat16 [2, 32, 64], P('gr', 'sp'), may hold values from -12 to 12
Outputs:
- kv_cache: bfloat16 [2, 32, 12288, 128], P('gr', 'sp', 'tp')
- gate_cache: float32 [2, 32, 12288], P('gr', 'sp', 'tp')
- read: bfloat16 [2, 32, 64], P('gr', 'sp')
The draws below stay inside these ranges and needn't reach their ends.
Inputs may be any that keep to these rules, and one draw needn't show every extreme that they name: `cum_gate`: each head's entries never rise along the positions.
All inputs are finite; a program needn't handle non-finite values.
Results may differ from the reference program's by a relative error of at most 0.012.
Values may be sent and summed in bfloat16 or wider, within the bound.
No kernel may reach another device: no remote copies, remote signals or barrier semaphores. Data moves between devices by JAX's collectives and lax.ppermute only.
A program may use at most 128 MiB of HBM per device.

```python
import jax
import jax.numpy as jnp

D = 2048
HEADS = 32
HD = 64
TOK_DEV = 768
SPAN = 6144
LEN = 12288
BATCH = 2
N_TP = 2


def draw_cum_gate(key, part):
    keys = jax.random.split(jax.random.fold_in(key, 7), 5)
    fast = jax.random.randint(keys[0], (BATCH, HEADS, 1), 0, 2) == 1
    spread = jnp.exp(jax.random.uniform(keys[1], (BATCH, HEADS, 1), jnp.float32, -0.7, 0.7))
    rate = jnp.where(fast, spread / 40.0, spread / LEN)
    blocks = LEN // TOK_DEV
    factor = jnp.exp(jax.random.uniform(keys[2], (BATCH, HEADS, blocks, 1), jnp.float32, -0.85, 0.85))
    factor = jnp.broadcast_to(factor, (BATCH, HEADS, blocks, TOK_DEV)).reshape(BATCH, HEADS, LEN)
    rough = jax.random.uniform(keys[3], (BATCH, HEADS, LEN), jnp.float32, 0.5, 1.5)
    log_gate = -rate * factor * rough
    start = -jax.random.uniform(keys[4], (BATCH, HEADS, 1), jnp.float32, 0.0, 300.0)
    total = start + jnp.cumsum(log_gate, axis=-1)
    return total.reshape(BATCH, HEADS, N_TP, SPAN).astype(jnp.float32)


def steps_of(key, shape, cuts, smallest, largest):
    factor_of, own = 1.0, jax.random.fold_in(key, 6)
    for axis_at, blocks in cuts:
        steps = jnp.exp(jax.random.uniform(jax.random.fold_in(own, axis_at), (blocks,), jnp.float32, smallest / len(cuts), largest / len(cuts)))
        factor_of = factor_of * jnp.repeat(steps, shape[axis_at] // blocks).reshape([-1 if axis == axis_at else 1 for axis in range(len(shape))])
    return factor_of


def normal_values(key, shape, scale, most, pieces=(), held_as=jnp.bfloat16):
    values = jax.random.normal(key, shape, jnp.float32) * scale
    if len(pieces) > 0:
        values = steps_of(key, shape, pieces, -0.22, 0.18) * values
    return jnp.clip(values, min=-most, max=most).astype(held_as)


def setup_inputs(seed: int = 0) -> dict:
    key_of = jax.random.split(jax.random.key(seed), 6)
    tokens = normal_values(key_of[0], (BATCH, N_TP, SPAN, D), 1.0, 6.0, ((0, 2), (1, 2), (2, 8)))
    key_weight = normal_values(key_of[1], (D, HEADS * HD), D ** -0.5, 0.125)
    value_weight = normal_values(key_of[2], (D, HEADS * HD), D ** -0.5, 0.125)
    cum_gate = draw_cum_gate(jax.random.fold_in(key_of[5], 71), 0)
    query = normal_values(key_of[4], (BATCH, HEADS, HD), 3.0, 12.0, ((0, 2), (1, 8)))
    return dict(tokens=tokens, key_weight=key_weight, value_weight=value_weight, cum_gate=cum_gate, query=query)


def reference(tokens, key_weight, value_weight, cum_gate, query):
    count = tokens.shape[0]
    rows = tokens.reshape(count * LEN, D)

    def project(weight):
        out = jnp.dot(rows, weight, preferred_element_type=jnp.float32).astype(jnp.bfloat16)
        return jnp.transpose(out.reshape(count, LEN, HEADS, HD), (0, 2, 1, 3))

    keys = project(key_weight)
    values = project(value_weight)
    kv_cache = jnp.concatenate([keys, values], axis=-1)
    gate_cache = cum_gate.reshape(count, HEADS, LEN)
    scores = jnp.einsum("bhe,bhse->bhs", query.astype(jnp.float32), keys.astype(jnp.float32))
    scores = scores * (HD ** -0.5) - gate_cache
    top = jnp.max(scores, axis=-1, keepdims=True)
    weights = jnp.exp(scores - top)
    total = jnp.sum(weights, axis=-1)
    probs = weights.astype(jnp.bfloat16).astype(jnp.float32)
    weighted = jnp.einsum("bhs,bhse->bhe", probs, values.astype(jnp.float32))
    read = (weighted / total[..., None]).astype(jnp.bfloat16)
    return kv_cache, gate_cache, read
```

```python
import jax
import jax.numpy as jnp
from jax import lax
from jax.experimental import pallas as pl
from jax.experimental.pallas import tpu as pltpu
from jax.sharding import PartitionSpec as P


LANES = 128


def owned(columns, owner, width):
    sharers = columns.shape[1] // width
    mine = columns[:, :width]
    for at in range(1, sharers):
        mine = jnp.where(owner % sharers == at, columns[:, at * width : (at + 1) * width], mine)
    return mine


def project_block(owner_ref, tokens_ref, key_ref, value_ref, out_ref):
    heads, _, width = out_ref.shape
    size = width // 2
    rows = tokens_ref[...]
    keys = jnp.dot(rows, key_ref[...], preferred_element_type=jnp.float32)
    values = jnp.dot(rows, value_ref[...], preferred_element_type=jnp.float32)
    keys = owned(keys, owner_ref[0], heads * size).astype(out_ref.dtype)
    values = owned(values, owner_ref[0], heads * size).astype(out_ref.dtype)
    for head in range(heads):
        part = slice(head * size, (head + 1) * size)
        out_ref[head] = jnp.concatenate([keys[:, part], values[:, part]], axis=-1)


def project(owner, rows, key_weight, value_weight, heads, size, place=None, places=1):
    count, width = rows.shape
    tile = count // 3 if count % 48 == 0 else count
    tiles = count // tile
    columns = max(heads * size, LANES)
    sharers = columns // (heads * size)
    scalars = jnp.stack([owner, owner if place is None else place]).astype(jnp.int32)
    shift = 0 if place is None else tiles

    def out_index(i, s):
        return (0, s[1] * shift + i, 0)

    def weight_index(i, s):
        return (0, s[0] // sharers)

    return pl.pallas_call(
        project_block,
        grid_spec=pltpu.PrefetchScalarGridSpec(
            num_scalar_prefetch=1,
            grid=(tiles,),
            in_specs=[
                pl.BlockSpec((tile, width), lambda i, s: (i, 0)),
                pl.BlockSpec((width, columns), weight_index),
                pl.BlockSpec((width, columns), weight_index),
            ],
            out_specs=pl.BlockSpec((heads, tile, 2 * size), out_index),
        ),
        out_shape=jax.ShapeDtypeStruct((heads, count * places, 2 * size), rows.dtype),
        cost_estimate=pl.CostEstimate(
            flops=4 * count * width * columns,
            bytes_accessed=2 * (count * width + 2 * width * columns + 2 * count * columns),
            transcendentals=0,
        ),
        name="project",
    )(scalars, rows, key_weight, value_weight)


def read_blocks(owners_ref, query_ref, gates_ref, *refs):
    block_refs, out_ref = refs[:-1], refs[-1]
    heads, rows, width = block_refs[0].shape
    size = width // 2
    lanes = lax.broadcasted_iota(jnp.int32, (1, width), 1)
    for at, block_ref in enumerate(block_refs):
        owner = owners_ref[at]
        for head in range(heads):
            block = block_ref[head]
            query = jnp.broadcast_to(query_ref[owner, pl.ds(head, 1), :], (8, width))
            scores = lax.dot_general(
                query.astype(block.dtype), block, (((1,), (1,)), ((), ())), preferred_element_type=jnp.float32
            )
            scores = scores[0:1] * size ** (-0.5) - gates_ref[owner, pl.ds(head, 1), :]
            top = jnp.max(scores, axis=-1, keepdims=True)
            weights = jnp.exp(scores - top)
            total = jnp.sum(weights, axis=-1, keepdims=True)
            probs = jnp.broadcast_to(weights, (8, rows)).astype(block.dtype)
            weighted = jnp.dot(probs, block, preferred_element_type=jnp.float32)[0:1]
            row = jnp.where(lanes == 0, top, jnp.where(lanes == 1, total, weighted))
            out_ref[owner, pl.ds(head, 1), :] = row


def partial_reads(owners, queries, gates, blocks):
    places, heads, size = queries.shape
    rows = blocks[0].shape[1]
    queries = jnp.pad(queries.astype(jnp.float32), ((0, 0), (0, 0), (0, size)))
    whole = pl.BlockSpec(memory_space=pltpu.VMEM)
    return pl.pallas_call(
        read_blocks,
        in_specs=[pl.BlockSpec(memory_space=pltpu.SMEM)] + [whole] * (2 + len(blocks)),
        out_specs=whole,
        out_shape=jax.ShapeDtypeStruct((places, heads, 2 * size), jnp.float32),
        cost_estimate=pl.CostEstimate(
            flops=16 * places * heads * rows * 2 * size,
            bytes_accessed=2 * places * heads * rows * 2 * size,
            transcendentals=places * heads * rows,
        ),
        name="read",
    )(owners, queries, gates, *blocks)


def merged_reads(parts, size):
    tops = parts[:, :, 0:1]
    top = jnp.max(tops, axis=0, keepdims=True)
    scale = jnp.exp(tops - top)
    total = jnp.sum(parts[:, :, 1:2] * scale, axis=0)
    weighted = jnp.sum(parts[:, :, size:] * scale, axis=0)
    return weighted / total


def on_device(places, tokens, key_weight, value_weight, cum_gate, query):
    heads, size = query.shape[1:]
    rows = tokens[0, 0]
    count = rows.shape[0]
    me = lax.axis_index("sp")
    far = places // 2
    near = [step for step in range(1, far)]
    steps = [far] + near[::-1] + [far + step for step in range(1, far)]

    def swap(value, step):
        return lax.ppermute(value, "sp", [(i, i ^ step) for i in range(places)])

    def block_of(owner):
        return project(owner, rows, key_weight, value_weight, heads, size)

    gates = cum_gate[0, :, 0, :].reshape(places, heads, count)
    queries = lax.all_to_all(
        jnp.broadcast_to(query, (places, heads, size)), "sp", split_axis=0, concat_axis=0, tiled=True
    )
    gate_parts = lax.all_to_all(gates, "sp", split_axis=0, concat_axis=0, tiled=True)
    gate_cache = jnp.transpose(gate_parts, (1, 0, 2)).reshape(1, heads, places * count)

    sent = {step: block_of(me ^ step) for step in steps}
    arrived = {step: swap(sent[step], step) for step in steps}
    cache = project(me, rows, key_weight, value_weight, heads, size, place=me, places=places)
    own = lax.dynamic_slice_in_dim(cache, me * count, count, 1)
    for step in steps:
        cache = lax.dynamic_update_slice_in_dim(cache, arrived[step], (me ^ step) * count, 1)

    owners = jnp.stack([me] + [me ^ step for step in steps]).astype(jnp.int32)
    parts = partial_reads(owners, queries, gates, [own] + [sent[step] for step in steps])
    parts = lax.all_to_all(parts, "sp", split_axis=0, concat_axis=0, tiled=True)
    parts = lax.all_gather(parts, "tp", tiled=True)
    read = merged_reads(parts, size).astype(jnp.bfloat16)[None]
    return (cache[None], gate_cache, read)


def solution(mesh):
    placed = (P("gr", "tp", "sp", None), P(), P(), P("gr", None, "tp", "sp"), P("gr", "sp", None))
    places = mesh.shape["sp"]

    def body(*args):
        return on_device(places, *args)

    return jax.shard_map(
        body,
        mesh=mesh,
        in_specs=placed,
        out_specs=(P("gr", "sp", "tp", None), P("gr", "sp", "tp"), P("gr", "sp", None)),
        check_vma=False,
    )
```

```python
import functools
import math

import jax
import jax.numpy as jnp
from jax import lax
from jax.experimental import pallas as pl
from jax.experimental.pallas import tpu as pltpu
from jax.sharding import PartitionSpec as P

LANES = 128
TILE = 384


def owned(columns, owner, width):
    sharers = columns.shape[1] // width
    mine = columns[:, :width]
    for at in range(1, sharers):
        mine = jnp.where(owner % sharers == at, columns[:, at * width : (at + 1) * width], mine)
    return mine


def project_block(step, me_ref, tokens_ref, key_ref, value_ref, out_ref):
    heads, _, width = out_ref.shape
    size = width // 2
    owner = me_ref[0] ^ step
    rows = tokens_ref[...]
    keys = jnp.dot(rows, key_ref[...], preferred_element_type=jnp.float32)
    values = jnp.dot(rows, value_ref[...], preferred_element_type=jnp.float32)
    keys = owned(keys, owner, heads * size).astype(out_ref.dtype)
    values = owned(values, owner, heads * size).astype(out_ref.dtype)
    for head in range(heads):
        part = slice(head * size, (head + 1) * size)
        out_ref[head] = jnp.concatenate([keys[:, part], values[:, part]], axis=-1)


def project(me, step, rows, key_weight, value_weight, heads, size, first=0, count=None, places=None):
    length, width = rows.shape
    count = length if count is None else count
    tile = math.gcd(count, math.gcd(first, TILE))
    tiles = count // tile
    columns = max(heads * size, LANES)
    sharers = columns // (heads * size)
    start = first // tile

    def out_index(i, s):
        return (0, i if places is None else s[0] * tiles + i, 0)

    def weight_index(i, s):
        return (0, (s[0] ^ step) // sharers)

    return pl.pallas_call(
        functools.partial(project_block, step),
        grid_spec=pltpu.PrefetchScalarGridSpec(
            num_scalar_prefetch=1,
            grid=(tiles,),
            in_specs=[
                pl.BlockSpec((tile, width), lambda i, s: (start + i, 0)),
                pl.BlockSpec((width, columns), weight_index),
                pl.BlockSpec((width, columns), weight_index),
            ],
            out_specs=pl.BlockSpec((heads, tile, 2 * size), out_index),
        ),
        out_shape=jax.ShapeDtypeStruct((heads, count * (places or 1), 2 * size), rows.dtype),
        cost_estimate=pl.CostEstimate(
            flops=4 * count * width * columns,
            bytes_accessed=2 * (count * width + 2 * width * columns + 2 * count * columns),
            transcendentals=0,
        ),
        name="project",
    )(me, rows, key_weight, value_weight)


def place_block(step, first, length, me_ref, block_ref, old_ref, out_ref, held, arrived, left):
    del old_ref
    heads, count, _ = block_ref.shape
    start = pl.multiple_of((me_ref[0] ^ step) * length + first, LANES)
    reads = [pltpu.make_async_copy(block_ref.at[head], held.at[head], arrived.at[head]) for head in range(heads)]
    writes = [
        pltpu.make_async_copy(held.at[head], out_ref.at[head, pl.ds(start, count), :], left.at[head])
        for head in range(heads)
    ]
    for read in reads:
        read.start()
    for read, write in zip(reads, writes):
        read.wait()
        write.start()
    for write in writes:
        write.wait()


def place(me, cache, block, step, first, length):
    anywhere = pl.BlockSpec(memory_space=pl.ANY)
    return pl.pallas_call(
        functools.partial(place_block, step, first, length),
        in_specs=[pl.BlockSpec(memory_space=pltpu.SMEM), anywhere, anywhere],
        out_specs=anywhere,
        out_shape=jax.ShapeDtypeStruct(cache.shape, cache.dtype),
        scratch_shapes=[
            pltpu.VMEM(block.shape, block.dtype),
            pltpu.SemaphoreType.DMA((block.shape[0],)),
            pltpu.SemaphoreType.DMA((block.shape[0],)),
        ],
        input_output_aliases={2: 0},
        cost_estimate=pl.CostEstimate(flops=block.size, bytes_accessed=4 * block.size, transcendentals=0),
        name="place",
    )(me, block, cache)


def read_blocks(owners, me_ref, query_ref, gates_ref, *refs):
    block_refs, out_ref = list(refs[:-1]), refs[-1]
    heads, _, width = block_refs[0].shape
    size = width // 2
    lanes = lax.broadcasted_iota(jnp.int32, (1, width), 1)
    for step, starts in owners:
        owner = me_ref[0] ^ step
        pieces = [(first, block_refs.pop(0)) for first in starts]
        for head in range(heads):
            query = jnp.broadcast_to(query_ref[owner, pl.ds(head, 1), :], (8, width))
            scores = []
            for first, block_ref in pieces:
                block = block_ref[head]
                score = lax.dot_general(
                    query.astype(block.dtype), block, (((1,), (1,)), ((), ())), preferred_element_type=jnp.float32
                )
                gates = gates_ref[owner, pl.ds(head, 1), pl.ds(first, block.shape[0])]
                scores.append(score[0:1] * size ** (-0.5) - gates)
            top = functools.reduce(jnp.maximum, [jnp.max(score, axis=-1, keepdims=True) for score in scores])
            total, weighted = 0.0, 0.0
            for (first, block_ref), score in zip(pieces, scores):
                weights = jnp.exp(score - top)
                total += jnp.sum(weights, axis=-1, keepdims=True)
                probs = jnp.broadcast_to(weights, (8, weights.shape[1])).astype(block_ref.dtype)
                weighted += jnp.dot(probs, block_ref[head], preferred_element_type=jnp.float32)[0:1]
            row = jnp.where(lanes == 0, top, jnp.where(lanes == 1, total, weighted))
            out_ref[owner, pl.ds(head, 1), :] = row


def partial_reads(me, owners, queries, gates, blocks):
    places, heads, size = queries.shape
    rows = gates.shape[2]
    queries = jnp.pad(queries.astype(jnp.float32), ((0, 0), (0, 0), (0, size)))
    whole = pl.BlockSpec(memory_space=pltpu.VMEM)
    return pl.pallas_call(
        functools.partial(read_blocks, owners),
        in_specs=[pl.BlockSpec(memory_space=pltpu.SMEM)] + [whole] * (2 + len(blocks)),
        out_specs=whole,
        out_shape=jax.ShapeDtypeStruct((places, heads, 2 * size), jnp.float32),
        cost_estimate=pl.CostEstimate(
            flops=16 * places * heads * rows * 2 * size,
            bytes_accessed=2 * places * heads * rows * 2 * size,
            transcendentals=places * heads * rows,
        ),
        name="read",
    )(me, queries, gates, *blocks)


def merged_reads(parts, size):
    tops = parts[:, :, 0:1]
    top = jnp.max(tops, axis=0, keepdims=True)
    scale = jnp.exp(tops - top)
    total = jnp.sum(parts[:, :, 1:2] * scale, axis=0)
    weighted = jnp.sum(parts[:, :, size:] * scale, axis=0)
    return weighted / total


def plan(places, rows):
    far = places // 2
    cut = rows // 2 // LANES * LANES
    early = [(far, 0, cut), (far, cut, rows - cut)] if cut else [(far, 0, rows)]
    late = list(range(far + 1, places))
    middle = late[: len(late) // 3]
    near = list(range(far - 1, 0, -1))
    order = near + middle
    return early, [(step, 0, rows) for step in order], [(step, 0, rows) for step in late[len(middle) :]]


def on_device(places, tokens, key_weight, value_weight, cum_gate, query):
    heads, size = query.shape[1:]
    rows = tokens[0, 0]
    length = rows.shape[0]
    me = lax.axis_index("sp").astype(jnp.int32).reshape(1)
    early, middle, late = plan(places, length)

    def swap(value, step):
        return lax.ppermute(value, "sp", [(i, i ^ step) for i in range(places)])

    def exchange(value):
        return lax.all_to_all(value, "sp", split_axis=0, concat_axis=0, tiled=True)

    sent, arrived = {}, {}
    for piece in early + middle + late:
        step, first, count = piece
        sent[piece] = project(me, step, rows, key_weight, value_weight, heads, size, first, count)
        arrived[piece] = swap(sent[piece], step)

    gates = cum_gate[0, :, 0, :].reshape(places, heads, length)
    asked = jnp.broadcast_to(query.astype(gates.dtype), (places, heads, size))
    gate_parts = exchange(jnp.concatenate([gates, asked], axis=-1))
    queries = gate_parts[:, :, length:]
    gate_parts = gate_parts[:, :, :length]
    gate_cache = jnp.transpose(gate_parts, (1, 0, 2)).reshape(1, heads, places * length)

    cache = project(me, 0, rows, key_weight, value_weight, heads, size, places=places)
    own = lax.dynamic_slice_in_dim(cache, me[0] * length, length, 1)

    steps = [early[0][0]] + [step for step, _, _ in middle + late]
    owners = [(0, [0])] + [(step, [piece[1] for piece in sent if piece[0] == step]) for step in steps]
    blocks = [own] + [sent[piece] for step in steps for piece in sent if piece[0] == step]
    parts = partial_reads(me, owners, queries, gates, blocks)
    parts = exchange(parts)
    parts = lax.all_gather(parts, "tp", tiled=True)
    read = merged_reads(parts, size).astype(jnp.bfloat16)[None]

    for step, first, _ in early + middle + late:
        cache = place(me, cache, arrived[(step, first, _)], step, first, length)
    return (cache[None], gate_cache, read)


def solution(mesh):
    placed = (P("gr", "tp", "sp", None), P(), P(), P("gr", None, "tp", "sp"), P("gr", "sp", None))
    places = mesh.shape["sp"]

    def body(*args):
        return on_device(places, *args)

    return jax.shard_map(
        body,
        mesh=mesh,
        in_specs=placed,
        out_specs=(P("gr", "sp", "tp", None), P("gr", "sp", "tp"), P("gr", "sp", None)),
        check_vma=False,
    )
```

```python
import functools

import jax
import jax.numpy as jnp
from jax import lax
from jax.experimental import pallas as pl
from jax.experimental.pallas import tpu as pltpu
from jax.sharding import PartitionSpec as P

LANES = 128
ROWS = 64
MIB = 1 << 20


def owned(columns, owner, width):
    sharers = columns.shape[1] // width
    mine = columns[:, :width]
    for at in range(1, sharers):
        mine = jnp.where(owner % sharers == at, columns[:, at * width : (at + 1) * width], mine)
    return mine


def project_block(step, me_ref, tokens_ref, key_ref, value_ref, out_ref):
    heads, _, width = out_ref.shape
    size = width // 2
    owner = me_ref[0] ^ step
    rows = tokens_ref[...]
    keys = jnp.dot(rows, key_ref[...], preferred_element_type=jnp.float32)
    values = jnp.dot(rows, value_ref[...], preferred_element_type=jnp.float32)
    keys = owned(keys, owner, heads * size).astype(out_ref.dtype)
    values = owned(values, owner, heads * size).astype(out_ref.dtype)
    for head in range(heads):
        part = slice(head * size, (head + 1) * size)
        out_ref[head] = jnp.concatenate([keys[:, part], values[:, part]], axis=-1)


def project(me, step, rows, count, key_weight, value_weight, heads, size):
    width = rows.shape[1]
    tiles = 2 if count % 32 == 0 else 1
    tile = count // tiles
    columns = max(heads * size, LANES)
    sharers = columns // (heads * size)

    def weight_index(i, s):
        return (0, (s[0] ^ step) // sharers)

    return pl.pallas_call(
        functools.partial(project_block, step),
        grid_spec=pltpu.PrefetchScalarGridSpec(
            num_scalar_prefetch=1,
            grid=(tiles,),
            in_specs=[
                pl.BlockSpec((tile, width), lambda i, s: (i, 0)),
                pl.BlockSpec((width, columns), weight_index),
                pl.BlockSpec((width, columns), weight_index),
            ],
            out_specs=pl.BlockSpec((heads, tile, 2 * size), lambda i, s: (0, i, 0)),
        ),
        out_shape=jax.ShapeDtypeStruct((heads, count, 2 * size), rows.dtype),
        cost_estimate=pl.CostEstimate(
            flops=4 * count * width * columns,
            bytes_accessed=2 * (count * width + 2 * width * columns + 2 * count * columns),
            transcendentals=0,
        ),
        name="project",
    )(me, rows, key_weight, value_weight)


def place_block(parts, length, block_ref, *refs):
    out_ref, left = refs[-2:]
    me = lax.axis_index("sp")
    writes = []
    for step, there, here, count in parts:
        start = pl.multiple_of((me ^ step) * length + there, ROWS)
        taken, put = block_ref.at[:, pl.ds(here, count), :], out_ref.at[:, pl.ds(start, count), :]
        writes.append(pltpu.make_async_copy(taken, put, left.at[len(writes)]))
    for write in writes:
        write.start()
    for write in writes:
        write.wait()


def place(cache, block, parts, places, length):
    heads, _, width = block.shape
    anywhere = pl.BlockSpec(memory_space=pl.ANY)
    old = () if cache is None else (cache,)
    return pl.pallas_call(
        functools.partial(place_block, parts, length),
        in_specs=[pl.BlockSpec(memory_space=pltpu.VMEM)] + [anywhere] * len(old),
        out_specs=anywhere,
        out_shape=jax.ShapeDtypeStruct((heads, places * length, width), block.dtype),
        scratch_shapes=[pltpu.SemaphoreType.DMA((len(parts),))],
        input_output_aliases={1: 0} if old else {},
        cost_estimate=pl.CostEstimate(flops=block.size, bytes_accessed=4 * block.size, transcendentals=0),
        compiler_params=pltpu.CompilerParams(vmem_limit_bytes=4 * MIB),
        name="place",
    )(block, *old)


def read_blocks(steps, near, me_ref, query_ref, gates_ref, borrowed_ref, *refs):
    block_refs, out_ref = refs[:-1], refs[-1]
    heads, _, width = block_refs[0].shape
    size = width // 2
    lanes = lax.broadcasted_iota(jnp.int32, (1, width), 1)
    for step, block_ref in zip(steps, block_refs):
        owner = me_ref[0] ^ step
        rows = block_ref.shape[1]
        for head in range(heads):
            block = block_ref[head]
            query = jnp.broadcast_to(query_ref[owner, pl.ds(head, 1), :], (8, width)).astype(block.dtype)
            scores = lax.dot_general(query, block, (((1,), (1,)), ((), ())), preferred_element_type=jnp.float32)
            gates = gates_ref[owner, pl.ds(head, 1), :]
            if step < near:
                more = borrowed_ref[lax.rem(owner, near), pl.ds(head, 1), :]
                gates = jnp.concatenate([gates, more], axis=-1)
            scores = scores[0:1] * size ** (-0.5) - gates[:, :rows]
            top = jnp.max(scores, axis=-1, keepdims=True)
            weights = jnp.exp(scores - top)
            total = jnp.sum(weights, axis=-1, keepdims=True)
            probs = jnp.broadcast_to(weights, (8, rows)).astype(block.dtype)
            weighted = jnp.dot(probs, block, preferred_element_type=jnp.float32)[0:1]
            row = jnp.where(lanes == 0, top, jnp.where(lanes == 1, total, weighted))
            out_ref[owner, pl.ds(head, 1), :] = row


def partial_reads(me, steps, near, queries, gates, borrowed, blocks):
    places, heads, size = queries.shape
    rows = gates.shape[2]
    queries = jnp.pad(queries.astype(jnp.float32), ((0, 0), (0, 0), (0, size)))
    whole = pl.BlockSpec(memory_space=pltpu.VMEM)
    return pl.pallas_call(
        functools.partial(read_blocks, steps, near),
        in_specs=[pl.BlockSpec(memory_space=pltpu.SMEM)] + [whole] * (3 + len(blocks)),
        out_specs=whole,
        out_shape=jax.ShapeDtypeStruct((places, heads, 2 * size), jnp.float32),
        cost_estimate=pl.CostEstimate(
            flops=16 * places * heads * rows * 2 * size,
            bytes_accessed=2 * places * heads * rows * 2 * size,
            transcendentals=places * heads * rows,
        ),
        name="read",
    )(me, queries, gates, borrowed, *blocks)


def merged_reads(parts, size):
    tops = parts[:, :, 0:1]
    top = jnp.max(tops, axis=0, keepdims=True)
    scale = jnp.exp(tops - top)
    total = jnp.sum(parts[:, :, 1:2] * scale, axis=0)
    weighted = jnp.sum(parts[:, :, size:] * scale, axis=0)
    return weighted / total


def plan(places):
    far = places // 2
    across, near = list(range(far, places)), list(range(1, far))
    half = len(across) // 2
    order = across[half:][::-1] + near + across[:half]
    return order[:-1], order[-1:]


def on_device(places, tokens, key_weight, value_weight, cum_gate, query):
    heads, size = query.shape[1:]
    rows = tokens[0, 0]
    length = rows.shape[0]
    far = places // 2
    me = lax.axis_index("sp").astype(jnp.int32)
    here = me.reshape(1)
    early, late = plan(places)
    kept = length - ROWS

    def swap(value, step):
        return lax.ppermute(value, "sp", [(i, i ^ step) for i in range(places)])

    def exchange(value):
        return lax.all_to_all(value, "sp", split_axis=0, concat_axis=0, tiled=True)

    lent = swap(rows[kept:], far)
    more = jnp.concatenate([rows, lent], axis=0)

    def block_of(step):
        mine, count = (more, length + ROWS) if step < far else (rows, kept)
        return project(here, step, mine, count, key_weight, value_weight, heads, size)

    def parts_of(step):
        if step < far:
            return ((step, 0, 0, length), (step ^ far, kept, length, ROWS))
        return ((step, 0, 0, kept),)

    sent, arrived = {}, {}
    for step in early + late:
        sent[step] = block_of(step)
        arrived[step] = swap(sent[step], step)

    gates = cum_gate[0, :, 0, :].reshape(places, heads, length)
    asked = jnp.broadcast_to(query.astype(gates.dtype), (places, heads, size))
    gate_parts = exchange(jnp.concatenate([gates, asked], axis=-1))
    queries = gate_parts[:, :, length:]
    gate_parts = gate_parts[:, :, :length]
    gate_cache = jnp.transpose(gate_parts, (1, 0, 2)).reshape(1, heads, places * length)
    borrowed = swap(lax.dynamic_slice(gates, ((me ^ far) & far, 0, kept), (far, heads, ROWS)), far)

    sent[0] = block_of(0)
    cache = place(None, sent[0], parts_of(0), places, length)
    steps = [0] + early + late
    parts = partial_reads(here, steps, far, queries, gates, borrowed, [sent[step] for step in steps])
    parts = exchange(parts)
    parts = lax.all_gather(parts, "tp", tiled=True)
    read = merged_reads(parts, size).astype(jnp.bfloat16)[None]

    for step in early + late:
        if step == late[-1]:
            cache, read = lax.optimization_barrier((cache, read))
        cache = place(cache, arrived[step], parts_of(step), places, length)
    return (cache[None], gate_cache, read)


def solution(mesh):
    placed = (P("gr", "tp", "sp", None), P(), P(), P("gr", None, "tp", "sp"), P("gr", "sp", None))
    places = mesh.shape["sp"]

    def body(*args):
        return on_device(places, *args)

    return jax.shard_map(
        body,
        mesh=mesh,
        in_specs=placed,
        out_specs=(P("gr", "sp", "tp", None), P("gr", "sp", "tp"), P("gr", "sp", None)),
        check_vma=False,
    )
```

```python
import functools

import jax
import jax.numpy as jnp
from jax import lax
from jax.experimental import pallas as pl
from jax.experimental.pallas import tpu as pltpu
from jax.sharding import PartitionSpec as P

LANES = 128
ROWS = 64
TAIL = 192
MIB = 1 << 20


def owned(columns, owner, width):
    sharers = columns.shape[1] // width
    mine = columns[:, :width]
    for at in range(1, sharers):
        mine = jnp.where(owner % sharers == at, columns[:, at * width : (at + 1) * width], mine)
    return mine


def project_block(step, me_ref, tokens_ref, key_ref, value_ref, out_ref):
    heads, _, width = out_ref.shape
    size = width // 2
    owner = me_ref[0] ^ step
    rows = tokens_ref[...]
    keys = jnp.dot(rows, key_ref[...], preferred_element_type=jnp.float32)
    values = jnp.dot(rows, value_ref[...], preferred_element_type=jnp.float32)
    keys = owned(keys, owner, heads * size).astype(out_ref.dtype)
    values = owned(values, owner, heads * size).astype(out_ref.dtype)
    for head in range(heads):
        part = slice(head * size, (head + 1) * size)
        out_ref[head] = jnp.concatenate([keys[:, part], values[:, part]], axis=-1)


def project(me, step, rows, count, key_weight, value_weight, heads, size):
    width = rows.shape[1]
    tiles = 2 if count % 32 == 0 else 1
    tile = count // tiles
    columns = max(heads * size, LANES)
    sharers = columns // (heads * size)

    def weight_index(i, s):
        return (0, (s[0] ^ step) // sharers)

    return pl.pallas_call(
        functools.partial(project_block, step),
        grid_spec=pltpu.PrefetchScalarGridSpec(
            num_scalar_prefetch=1,
            grid=(tiles,),
            in_specs=[
                pl.BlockSpec((tile, width), lambda i, s: (i, 0)),
                pl.BlockSpec((width, columns), weight_index),
                pl.BlockSpec((width, columns), weight_index),
            ],
            out_specs=pl.BlockSpec((heads, tile, 2 * size), lambda i, s: (0, i, 0)),
        ),
        out_shape=jax.ShapeDtypeStruct((heads, count, 2 * size), rows.dtype),
        cost_estimate=pl.CostEstimate(
            flops=4 * count * width * columns,
            bytes_accessed=2 * (count * width + 2 * width * columns + 2 * count * columns),
            transcendentals=0,
        ),
        name="project",
    )(me, rows, key_weight, value_weight)


def place_block(parts, length, block_ref, *refs):
    out_ref, left = refs[-2:]
    me = lax.axis_index("sp")
    writes = []
    for step, there, here, count in parts:
        start = pl.multiple_of((me ^ step) * length + there, ROWS)
        taken, put = block_ref.at[:, pl.ds(here, count), :], out_ref.at[:, pl.ds(start, count), :]
        writes.append(pltpu.make_async_copy(taken, put, left.at[len(writes)]))
    for write in writes:
        write.start()
    for write in writes:
        write.wait()


def place(cache, block, parts, places, length):
    heads, _, width = block.shape
    anywhere = pl.BlockSpec(memory_space=pl.ANY)
    old = () if cache is None else (cache,)
    return pl.pallas_call(
        functools.partial(place_block, parts, length),
        in_specs=[pl.BlockSpec(memory_space=pltpu.VMEM)] + [anywhere] * len(old),
        out_specs=anywhere,
        out_shape=jax.ShapeDtypeStruct((heads, places * length, width), block.dtype),
        scratch_shapes=[pltpu.SemaphoreType.DMA((len(parts),))],
        input_output_aliases={1: 0} if old else {},
        cost_estimate=pl.CostEstimate(flops=block.size, bytes_accessed=4 * block.size, transcendentals=0),
        compiler_params=pltpu.CompilerParams(vmem_limit_bytes=4 * MIB),
        name="place",
    )(block, *old)


def read_blocks(steps, near, me_ref, query_ref, gates_ref, borrowed_ref, *refs):
    block_refs, out_ref = refs[:-1], refs[-1]
    heads, _, width = block_refs[0].shape
    size = width // 2
    lanes = lax.broadcasted_iota(jnp.int32, (1, width), 1)
    for step, block_ref in zip(steps, block_refs):
        owner = me_ref[0] ^ step
        rows = block_ref.shape[1]
        for head in range(heads):
            block = block_ref[head]
            query = jnp.broadcast_to(query_ref[owner, pl.ds(head, 1), :], (8, width)).astype(block.dtype)
            scores = lax.dot_general(query, block, (((1,), (1,)), ((), ())), preferred_element_type=jnp.float32)
            gates = gates_ref[owner, pl.ds(head, 1), :]
            if step < near:
                more = borrowed_ref[lax.rem(owner, near), pl.ds(head, 1), :]
                gates = jnp.concatenate([gates, more], axis=-1)
            scores = scores[0:1] * size ** (-0.5) - gates[:, :rows]
            top = jnp.max(scores, axis=-1, keepdims=True)
            weights = jnp.exp(scores - top)
            total = jnp.sum(weights, axis=-1, keepdims=True)
            probs = jnp.broadcast_to(weights, (8, rows)).astype(block.dtype)
            weighted = jnp.dot(probs, block, preferred_element_type=jnp.float32)[0:1]
            row = jnp.where(lanes == 0, top, jnp.where(lanes == 1, total, weighted))
            out_ref[owner, pl.ds(head, 1), :] = row


def partial_reads(me, steps, near, queries, gates, borrowed, blocks):
    places, heads, size = queries.shape
    rows = gates.shape[2]
    queries = jnp.pad(queries.astype(jnp.float32), ((0, 0), (0, 0), (0, size)))
    whole = pl.BlockSpec(memory_space=pltpu.VMEM)
    return pl.pallas_call(
        functools.partial(read_blocks, steps, near),
        in_specs=[pl.BlockSpec(memory_space=pltpu.SMEM)] + [whole] * (3 + len(blocks)),
        out_specs=whole,
        out_shape=jax.ShapeDtypeStruct((places, heads, 2 * size), jnp.float32),
        cost_estimate=pl.CostEstimate(
            flops=16 * places * heads * rows * 2 * size,
            bytes_accessed=2 * places * heads * rows * 2 * size,
            transcendentals=places * heads * rows,
        ),
        name="read",
    )(me, queries, gates, borrowed, *blocks)


def merged_reads(parts, size):
    tops = parts[:, :, 0:1]
    top = jnp.max(tops, axis=0, keepdims=True)
    scale = jnp.exp(tops - top)
    total = jnp.sum(parts[:, :, 1:2] * scale, axis=0)
    weighted = jnp.sum(parts[:, :, size:] * scale, axis=0)
    return weighted / total


def packed_gates(gates):
    places, heads, length = gates.shape
    groups = gates.reshape(places, heads, length // LANES, LANES)
    first = groups[..., :1]
    falls = (groups - first).astype(jnp.bfloat16).reshape(gates.shape)
    rest, terms = first[..., 0], []
    for _ in range(3):
        terms.append(lax.reduce_precision(rest, 8, 7))
        rest = rest - terms[-1]
    return jnp.concatenate([falls] + [term.astype(jnp.bfloat16) for term in terms], axis=-1)


def unpacked_gates(packed, length):
    places, heads, _ = packed.shape
    packed = packed.astype(jnp.float32)
    falls, terms = packed[..., :length], packed[..., length:]
    first = jnp.sum(terms.reshape(places, heads, 3, length // LANES), axis=2)
    groups = falls.reshape(places, heads, length // LANES, LANES) + first[..., None]
    return groups.reshape(places, heads, length)


def plan(places):
    far = places // 2
    across, near = list(range(far, places)), list(range(1, far))
    half = len(across) // 2
    order = across[half:][::-1] + near + across[:half]
    return order[:-1], order[-1:]


def on_device(places, tokens, key_weight, value_weight, cum_gate, query):
    heads, size = query.shape[1:]
    rows = tokens[0, 0]
    length = rows.shape[0]
    far = places // 2
    me = lax.axis_index("sp").astype(jnp.int32)
    here = me.reshape(1)
    early, late = plan(places)
    kept = length - ROWS

    def swap(value, step):
        return lax.ppermute(value, "sp", [(i, i ^ step) for i in range(places)])

    def exchange(value):
        return lax.all_to_all(value, "sp", split_axis=0, concat_axis=0, tiled=True)

    lent = swap(rows[kept:], far)
    more = jnp.concatenate([rows, lent], axis=0)

    def block_of(step):
        mine, count = (more, length + ROWS) if step < far else (rows, kept)
        return project(here, step, mine, count, key_weight, value_weight, heads, size)

    def parts_of(step):
        if step < far:
            return ((step, 0, 0, length), (step ^ far, kept, length, ROWS))
        return ((step, 0, 0, kept),)

    sent, arrived = {}, []
    for step in early + late:
        sent[step] = block_of(step)
        pieces = [("", sent[step], parts_of(step))]
        if step in late:
            head = kept - TAIL
            pieces = [
                ("", sent[step][:, :head], ((step, 0, 0, head),)),
                ("_tail", sent[step][:, head:], ((step, head, 0, TAIL),)),
            ]
        for name, block, parts in pieces:
            arrived.append((f"place_{step}{name}", swap(block, step), parts))

    gates = cum_gate[0, :, 0, :].reshape(places, heads, length)
    asked = jnp.broadcast_to(query, (places, heads, size))
    told = exchange(jnp.concatenate([packed_gates(gates), asked], axis=-1))
    queries = told[:, :, -size:]
    gate_parts = unpacked_gates(told[:, :, :-size], length)
    gate_cache = jnp.transpose(gate_parts, (1, 0, 2)).reshape(1, heads, places * length)
    borrowed = swap(lax.dynamic_slice(gates, ((me ^ far) & far, 0, kept), (far, heads, ROWS)), far)

    sent[0] = block_of(0)
    cache = place(None, sent[0], parts_of(0), places, length)
    steps = [0] + early + late
    parts = partial_reads(here, steps, far, queries, gates, borrowed, [sent[step] for step in steps])
    parts = exchange(parts)
    parts = lax.all_gather(parts, "tp", tiled=True)
    read = merged_reads(parts, size).astype(jnp.bfloat16)[None]

    for name, block, parts in arrived:
        if name == f"place_{late[-1]}":
            cache, read = lax.optimization_barrier((cache, read))
        cache = place(cache, block, parts, places, length)
    return (cache[None], gate_cache, read)


def solution(mesh):
    placed = (P("gr", "tp", "sp", None), P(), P(), P("gr", None, "tp", "sp"), P("gr", "sp", None))
    places = mesh.shape["sp"]

    def body(*args):
        return on_device(places, *args)

    return jax.shard_map(
        body,
        mesh=mesh,
        in_specs=placed,
        out_specs=(P("gr", "sp", "tp", None), P("gr", "sp", "tp"), P("gr", "sp", None)),
        check_vma=False,
    )
```

```python
import functools

import jax
import jax.numpy as jnp
from jax import lax
from jax.experimental import pallas as pl
from jax.experimental.pallas import tpu as pltpu
from jax.sharding import PartitionSpec as P

LANES = 128
ROWS = 64
TAIL = 192
MIB = 1 << 20


def owned(columns, owner, width):
    sharers = columns.shape[1] // width
    mine = columns[:, :width]
    for at in range(1, sharers):
        mine = jnp.where(owner % sharers == at, columns[:, at * width : (at + 1) * width], mine)
    return mine


def project_block(step, me_ref, tokens_ref, key_ref, value_ref, out_ref):
    heads, _, width = out_ref.shape
    size = width // 2
    owner = me_ref[0] ^ step
    rows = tokens_ref[...]
    keys = jnp.dot(rows, key_ref[...], preferred_element_type=jnp.float32)
    values = jnp.dot(rows, value_ref[...], preferred_element_type=jnp.float32)
    keys = owned(keys, owner, heads * size).astype(out_ref.dtype)
    values = owned(values, owner, heads * size).astype(out_ref.dtype)
    for head in range(heads):
        part = slice(head * size, (head + 1) * size)
        out_ref[head] = jnp.concatenate([keys[:, part], values[:, part]], axis=-1)


def project(me, step, rows, count, key_weight, value_weight, heads, size):
    width = rows.shape[1]
    tiles = 2 if count % 32 == 0 else 1
    tile = count // tiles
    columns = max(heads * size, LANES)
    sharers = columns // (heads * size)

    def weight_index(i, s):
        return (0, (s[0] ^ step) // sharers)

    return pl.pallas_call(
        functools.partial(project_block, step),
        grid_spec=pltpu.PrefetchScalarGridSpec(
            num_scalar_prefetch=1,
            grid=(tiles,),
            in_specs=[
                pl.BlockSpec((tile, width), lambda i, s: (i, 0)),
                pl.BlockSpec((width, columns), weight_index),
                pl.BlockSpec((width, columns), weight_index),
            ],
            out_specs=pl.BlockSpec((heads, tile, 2 * size), lambda i, s: (0, i, 0)),
        ),
        out_shape=jax.ShapeDtypeStruct((heads, count, 2 * size), rows.dtype),
        cost_estimate=pl.CostEstimate(
            flops=4 * count * width * columns,
            bytes_accessed=2 * (count * width + 2 * width * columns + 2 * count * columns),
            transcendentals=0,
        ),
        name="project",
    )(me, rows, key_weight, value_weight)


def place_block(parts, length, block_ref, *refs):
    out_ref, left = refs[-2:]
    me = lax.axis_index("sp")
    writes = []
    for step, there, here, count in parts:
        start = pl.multiple_of((me ^ step) * length + there, ROWS)
        taken, put = block_ref.at[:, pl.ds(here, count), :], out_ref.at[:, pl.ds(start, count), :]
        writes.append(pltpu.make_async_copy(taken, put, left.at[len(writes)]))
    for write in writes:
        write.start()
    for write in writes:
        write.wait()


def place(cache, block, parts, places, length):
    heads, _, width = block.shape
    anywhere = pl.BlockSpec(memory_space=pl.ANY)
    old = () if cache is None else (cache,)
    return pl.pallas_call(
        functools.partial(place_block, parts, length),
        in_specs=[pl.BlockSpec(memory_space=pltpu.VMEM)] + [anywhere] * len(old),
        out_specs=anywhere,
        out_shape=jax.ShapeDtypeStruct((heads, places * length, width), block.dtype),
        scratch_shapes=[pltpu.SemaphoreType.DMA((len(parts),))],
        input_output_aliases={1: 0} if old else {},
        cost_estimate=pl.CostEstimate(flops=block.size, bytes_accessed=4 * block.size, transcendentals=0),
        compiler_params=pltpu.CompilerParams(vmem_limit_bytes=4 * MIB),
        name="place",
    )(block, *old)


def read_blocks(steps, near, me_ref, query_ref, gates_ref, borrowed_ref, *refs):
    block_refs, out_ref = refs[:-1], refs[-1]
    heads, _, width = block_refs[0].shape
    size = width // 2
    lanes = lax.broadcasted_iota(jnp.int32, (1, width), 1)
    for step, block_ref in zip(steps, block_refs):
        owner = me_ref[0] ^ step
        rows = block_ref.shape[1]
        for head in range(heads):
            block = block_ref[head]
            query = jnp.broadcast_to(query_ref[owner, pl.ds(head, 1), :], (8, width)).astype(block.dtype)
            scores = lax.dot_general(query, block, (((1,), (1,)), ((), ())), preferred_element_type=jnp.float32)
            gates = gates_ref[owner, pl.ds(head, 1), :]
            if step < near:
                more = borrowed_ref[lax.rem(owner, near), pl.ds(head, 1), :]
                gates = jnp.concatenate([gates, more], axis=-1)
            scores = scores[0:1] * size ** (-0.5) - gates[:, :rows]
            top = jnp.max(scores, axis=-1, keepdims=True)
            weights = jnp.exp(scores - top)
            total = jnp.sum(weights, axis=-1, keepdims=True)
            probs = jnp.broadcast_to(weights, (8, rows)).astype(block.dtype)
            weighted = jnp.dot(probs, block, preferred_element_type=jnp.float32)[0:1]
            row = jnp.where(lanes == 0, top, jnp.where(lanes == 1, total, weighted))
            out_ref[owner, pl.ds(head, 1), :] = row


def partial_reads(me, steps, near, queries, gates, borrowed, blocks):
    places, heads, size = queries.shape
    rows = gates.shape[2]
    queries = jnp.pad(queries.astype(jnp.float32), ((0, 0), (0, 0), (0, size)))
    whole = pl.BlockSpec(memory_space=pltpu.VMEM)
    return pl.pallas_call(
        functools.partial(read_blocks, steps, near),
        in_specs=[pl.BlockSpec(memory_space=pltpu.SMEM)] + [whole] * (3 + len(blocks)),
        out_specs=whole,
        out_shape=jax.ShapeDtypeStruct((places, heads, 2 * size), jnp.float32),
        cost_estimate=pl.CostEstimate(
            flops=16 * places * heads * rows * 2 * size,
            bytes_accessed=2 * places * heads * rows * 2 * size,
            transcendentals=places * heads * rows,
        ),
        name="read",
    )(me, queries, gates, borrowed, *blocks)


def merged_reads(parts, size):
    tops = parts[:, :, 0:1]
    top = jnp.max(tops, axis=0, keepdims=True)
    scale = jnp.exp(tops - top)
    total = jnp.sum(parts[:, :, 1:2] * scale, axis=0)
    weighted = jnp.sum(parts[:, :, size:] * scale, axis=0)
    return weighted / total


def packed_gates(gates):
    places, heads, length = gates.shape
    groups = gates.reshape(places, heads, length // LANES, LANES)
    first = groups[..., :1]
    falls = (groups - first).astype(jnp.bfloat16).reshape(gates.shape)
    rest, terms = first[..., 0], []
    for _ in range(3):
        terms.append(lax.reduce_precision(rest, 8, 7))
        rest = rest - terms[-1]
    return jnp.concatenate([falls] + [term.astype(jnp.bfloat16) for term in terms], axis=-1)


def unpacked_gates(packed, length):
    places, heads, _ = packed.shape
    packed = packed.astype(jnp.float32)
    falls, terms = packed[..., :length], packed[..., length:]
    first = jnp.sum(terms.reshape(places, heads, 3, length // LANES), axis=2)
    groups = falls.reshape(places, heads, length // LANES, LANES) + first[..., None]
    return groups.reshape(places, heads, length)


def plan(places):
    far = places // 2
    across = [places - 1] + list(range(far, places - 1))
    near = [far // 2] + [step for step in range(1, far) if step != far // 2]
    half = len(across) // 2
    order = across[:half] + near + across[half:]
    return order[:-1], order[-1:]


def on_device(places, tokens, key_weight, value_weight, cum_gate, query):
    heads, size = query.shape[1:]
    rows = tokens[0, 0]
    length = rows.shape[0]
    far = places // 2
    me = lax.axis_index("sp").astype(jnp.int32)
    here = me.reshape(1)
    early, late = plan(places)
    kept = length - ROWS

    def swap(value, step):
        return lax.ppermute(value, "sp", [(i, i ^ step) for i in range(places)])

    def exchange(value):
        return lax.all_to_all(value, "sp", split_axis=0, concat_axis=0, tiled=True)

    lent = swap(rows[kept:], far)
    more = jnp.concatenate([rows, lent], axis=0)

    def block_of(step):
        mine, count = (more, length + ROWS) if step < far else (rows, kept)
        return project(here, step, mine, count, key_weight, value_weight, heads, size)

    def parts_of(step):
        if step < far:
            return ((step, 0, 0, length), (step ^ far, kept, length, ROWS))
        return ((step, 0, 0, kept),)

    sent, arrived = {}, []
    for step in early + late:
        sent[step] = block_of(step)
        pieces = [("", sent[step], parts_of(step))]
        if step in late:
            head = kept - TAIL
            pieces = [
                ("", sent[step][:, :head], ((step, 0, 0, head),)),
                ("_tail", sent[step][:, head:], ((step, head, 0, TAIL),)),
            ]
        for name, block, parts in pieces:
            arrived.append((f"place_{step}{name}", swap(block, step), parts))

    gates = cum_gate[0, :, 0, :].reshape(places, heads, length)
    asked = jnp.broadcast_to(query, (places, heads, size))
    told = exchange(jnp.concatenate([packed_gates(gates), asked], axis=-1))
    queries = told[:, :, -size:]
    gate_parts = unpacked_gates(told[:, :, :-size], length)
    gate_cache = jnp.transpose(gate_parts, (1, 0, 2)).reshape(1, heads, places * length)
    borrowed = swap(lax.dynamic_slice(gates, ((me ^ far) & far, 0, kept), (far, heads, ROWS)), far)

    sent[0] = block_of(0)
    cache = place(None, sent[0], parts_of(0), places, length)
    steps = [0] + early + late
    parts = partial_reads(here, steps, far, queries, gates, borrowed, [sent[step] for step in steps])
    parts = exchange(parts)
    parts = lax.all_gather(parts, "tp", tiled=True)
    read = merged_reads(parts, size).astype(jnp.bfloat16)[None]

    for name, block, parts in arrived:
        if name == f"place_{late[-1]}":
            cache, read = lax.optimization_barrier((cache, read))
        cache = place(cache, block, parts, places, length)
    return (cache[None], gate_cache, read)


def solution(mesh):
    placed = (P("gr", "tp", "sp", None), P(), P(), P("gr", None, "tp", "sp"), P("gr", "sp", None))
    places = mesh.shape["sp"]

    def body(*args):
        return on_device(places, *args)

    return jax.shard_map(
        body,
        mesh=mesh,
        in_specs=placed,
        out_specs=(P("gr", "sp", "tp", None), P("gr", "sp", "tp"), P("gr", "sp", None)),
        check_vma=False,
    )
```

```python
import functools

import jax
import jax.numpy as jnp
from jax import lax
from jax.experimental import pallas as pl
from jax.experimental.pallas import tpu as pltpu
from jax.sharding import PartitionSpec as P

LANES = 128
ROWS = 64
TAIL = 192
MIB = 1 << 20


def owned(columns, owner, width):
    sharers = columns.shape[1] // width
    mine = columns[:, :width]
    for at in range(1, sharers):
        mine = jnp.where(owner % sharers == at, columns[:, at * width : (at + 1) * width], mine)
    return mine


def project_block(step, me_ref, tokens_ref, key_ref, value_ref, out_ref):
    heads, _, width = out_ref.shape
    size = width // 2
    owner = me_ref[0] ^ step
    rows = tokens_ref[...]
    keys = jnp.dot(rows, key_ref[...], preferred_element_type=jnp.float32)
    values = jnp.dot(rows, value_ref[...], preferred_element_type=jnp.float32)
    keys = owned(keys, owner, heads * size).astype(out_ref.dtype)
    values = owned(values, owner, heads * size).astype(out_ref.dtype)
    for head in range(heads):
        part = slice(head * size, (head + 1) * size)
        out_ref[head] = jnp.concatenate([keys[:, part], values[:, part]], axis=-1)


def project(me, step, rows, count, key_weight, value_weight, heads, size):
    width = rows.shape[1]
    tiles = 2 if count % 32 == 0 else 1
    tile = count // tiles
    columns = max(heads * size, LANES)
    sharers = columns // (heads * size)

    def weight_index(i, s):
        return (0, (s[0] ^ step) // sharers)

    return pl.pallas_call(
        functools.partial(project_block, step),
        grid_spec=pltpu.PrefetchScalarGridSpec(
            num_scalar_prefetch=1,
            grid=(tiles,),
            in_specs=[
                pl.BlockSpec((tile, width), lambda i, s: (i, 0)),
                pl.BlockSpec((width, columns), weight_index),
                pl.BlockSpec((width, columns), weight_index),
            ],
            out_specs=pl.BlockSpec((heads, tile, 2 * size), lambda i, s: (0, i, 0)),
        ),
        out_shape=jax.ShapeDtypeStruct((heads, count, 2 * size), rows.dtype),
        cost_estimate=pl.CostEstimate(
            flops=4 * count * width * columns,
            bytes_accessed=2 * (count * width + 2 * width * columns + 2 * count * columns),
            transcendentals=0,
        ),
        name="project",
    )(me, rows, key_weight, value_weight)


def place_block(parts, length, block_ref, *refs):
    out_ref, left = refs[-2:]
    me = lax.axis_index("sp")
    writes = []
    for step, there, here, count in parts:
        start = pl.multiple_of((me ^ step) * length + there, ROWS)
        taken, put = block_ref.at[:, pl.ds(here, count), :], out_ref.at[:, pl.ds(start, count), :]
        writes.append(pltpu.make_async_copy(taken, put, left.at[len(writes)]))
    for write in writes:
        write.start()
    for write in writes:
        write.wait()


def place(cache, block, parts, places, length):
    heads, _, width = block.shape
    anywhere = pl.BlockSpec(memory_space=pl.ANY)
    old = () if cache is None else (cache,)
    return pl.pallas_call(
        functools.partial(place_block, parts, length),
        in_specs=[pl.BlockSpec(memory_space=pltpu.VMEM)] + [anywhere] * len(old),
        out_specs=anywhere,
        out_shape=jax.ShapeDtypeStruct((heads, places * length, width), block.dtype),
        scratch_shapes=[pltpu.SemaphoreType.DMA((len(parts),))],
        input_output_aliases={1: 0} if old else {},
        cost_estimate=pl.CostEstimate(flops=block.size, bytes_accessed=4 * block.size, transcendentals=0),
        compiler_params=pltpu.CompilerParams(vmem_limit_bytes=4 * MIB),
        name="place",
    )(block, *old)


def read_blocks(steps, near, me_ref, query_ref, gates_ref, borrowed_ref, *refs):
    block_refs, out_ref = refs[:-1], refs[-1]
    heads, _, width = block_refs[0].shape
    size = width // 2
    lanes = lax.broadcasted_iota(jnp.int32, (1, width), 1)
    for step, block_ref in zip(steps, block_refs):
        owner = me_ref[0] ^ step
        rows = block_ref.shape[1]
        for head in range(heads):
            block = block_ref[head]
            query = jnp.broadcast_to(query_ref[owner, pl.ds(head, 1), :], (8, width)).astype(block.dtype)
            scores = lax.dot_general(query, block, (((1,), (1,)), ((), ())), preferred_element_type=jnp.float32)
            gates = gates_ref[owner, pl.ds(head, 1), :]
            if step < near:
                more = borrowed_ref[lax.rem(owner, near), pl.ds(head, 1), :]
                gates = jnp.concatenate([gates, more], axis=-1)
            scores = scores[0:1] * size ** (-0.5) - gates[:, :rows]
            top = jnp.max(scores, axis=-1, keepdims=True)
            weights = jnp.exp(scores - top)
            total = jnp.sum(weights, axis=-1, keepdims=True)
            probs = jnp.broadcast_to(weights, (8, rows)).astype(block.dtype)
            weighted = jnp.dot(probs, block, preferred_element_type=jnp.float32)[0:1]
            row = jnp.where(lanes == 0, top, jnp.where(lanes == 1, total, weighted))
            out_ref[owner, pl.ds(head, 1), :] = row


def partial_reads(me, steps, near, queries, gates, borrowed, blocks):
    places, heads, size = queries.shape
    rows = gates.shape[2]
    queries = jnp.pad(queries.astype(jnp.float32), ((0, 0), (0, 0), (0, size)))
    whole = pl.BlockSpec(memory_space=pltpu.VMEM)
    return pl.pallas_call(
        functools.partial(read_blocks, steps, near),
        in_specs=[pl.BlockSpec(memory_space=pltpu.SMEM)] + [whole] * (3 + len(blocks)),
        out_specs=whole,
        out_shape=jax.ShapeDtypeStruct((places, heads, 2 * size), jnp.float32),
        cost_estimate=pl.CostEstimate(
            flops=16 * places * heads * rows * 2 * size,
            bytes_accessed=2 * places * heads * rows * 2 * size,
            transcendentals=places * heads * rows,
        ),
        name="read",
    )(me, queries, gates, borrowed, *blocks)


def merged_reads(parts, size):
    tops = parts[:, :, 0:1]
    top = jnp.max(tops, axis=0, keepdims=True)
    scale = jnp.exp(tops - top)
    total = jnp.sum(parts[:, :, 1:2] * scale, axis=0)
    weighted = jnp.sum(parts[:, :, size:] * scale, axis=0)
    return weighted / total


def packed_gates(gates):
    places, heads, length = gates.shape
    groups = gates.reshape(places, heads, length // LANES, LANES)
    first = groups[..., :1]
    falls = (groups - first).astype(jnp.bfloat16).reshape(gates.shape)
    rest, terms = first[..., 0], []
    for _ in range(3):
        terms.append(lax.reduce_precision(rest, 8, 7))
        rest = rest - terms[-1]
    return jnp.concatenate([falls] + [term.astype(jnp.bfloat16) for term in terms], axis=-1)


def unpacked_gates(packed, length):
    places, heads, _ = packed.shape
    packed = packed.astype(jnp.float32)
    falls, terms = packed[..., :length], packed[..., length:]
    first = jnp.sum(terms.reshape(places, heads, 3, length // LANES), axis=2)
    groups = falls.reshape(places, heads, length // LANES, LANES) + first[..., None]
    return groups.reshape(places, heads, length)


def plan(places):
    far = places // 2
    across = [places - 1] + list(range(far, places - 1))
    near = [far // 2] + [step for step in range(1, far) if step != far // 2]
    half = len(across) // 2
    order = across[:half] + near + across[half:]
    return order[:-1], order[-1:]


def on_device(places, tokens, key_weight, value_weight, cum_gate, query):
    heads, size = query.shape[1:]
    rows = tokens[0, 0]
    length = rows.shape[0]
    far = places // 2
    peer = far + far // 2
    me = lax.axis_index("sp").astype(jnp.int32)
    here = me.reshape(1)
    early, late = plan(places)
    kept = length - ROWS

    def swap(value, step):
        return lax.ppermute(value, "sp", [(i, i ^ step) for i in range(places)])

    def exchange(value):
        return lax.all_to_all(value, "sp", split_axis=0, concat_axis=0, tiled=True)

    lent = swap(rows[kept:], peer)
    more = jnp.concatenate([rows, lent], axis=0)

    def block_of(step):
        mine, count = (more, length + ROWS) if step < far else (rows, kept)
        return project(here, step, mine, count, key_weight, value_weight, heads, size)

    def parts_of(step):
        if step < far:
            return ((step, 0, 0, length), (step ^ peer, kept, length, ROWS))
        return ((step, 0, 0, kept),)

    sent, arrived = {}, []
    for step in early + late:
        sent[step] = block_of(step)
        pieces = [("", sent[step], parts_of(step))]
        if step in late:
            head = kept - TAIL
            pieces = [
                ("", sent[step][:, :head], ((step, 0, 0, head),)),
                ("_tail", sent[step][:, head:], ((step, head, 0, TAIL),)),
            ]
        for name, block, parts in pieces:
            arrived.append((f"place_{step}{name}", swap(block, step), parts))

    gates = cum_gate[0, :, 0, :].reshape(places, heads, length)
    asked = jnp.broadcast_to(query, (places, heads, size))
    told = exchange(jnp.concatenate([packed_gates(gates), asked], axis=-1))
    queries = told[:, :, -size:]
    gate_parts = unpacked_gates(told[:, :, :-size], length)
    gate_cache = jnp.transpose(gate_parts, (1, 0, 2)).reshape(1, heads, places * length)
    borrowed = swap(lax.dynamic_slice(gates, ((me ^ far) & far, 0, kept), (far, heads, ROWS)), peer)

    sent[0] = block_of(0)
    cache = place(None, sent[0], parts_of(0), places, length)
    steps = [0] + early + late
    parts = partial_reads(here, steps, far, queries, gates, borrowed, [sent[step] for step in steps])
    parts = exchange(parts)
    parts = lax.all_gather(parts, "tp", tiled=True)
    read = merged_reads(parts, size).astype(jnp.bfloat16)[None]

    for name, block, parts in arrived:
        if name == f"place_{late[-1]}":
            cache, read = lax.optimization_barrier((cache, read))
        cache = place(cache, block, parts, places, length)
    return (cache[None], gate_cache, read)


def solution(mesh):
    placed = (P("gr", "tp", "sp", None), P(), P(), P("gr", None, "tp", "sp"), P("gr", "sp", None))
    places = mesh.shape["sp"]

    def body(*args):
        return on_device(places, *args)

    return jax.shard_map(
        body,
        mesh=mesh,
        in_specs=placed,
        out_specs=(P("gr", "sp", "tp", None), P("gr", "sp", "tp"), P("gr", "sp", None)),
        check_vma=False,
    )
```

```python
import functools

import jax
import jax.numpy as jnp
from jax import lax
from jax.experimental import pallas as pl
from jax.experimental.pallas import tpu as pltpu
from jax.sharding import PartitionSpec as P

LANES = 128
ROWS = 64
TAIL = 128
MIB = 1 << 20


def owned(columns, owner, width):
    sharers = columns.shape[1] // width
    mine = columns[:, :width]
    for at in range(1, sharers):
        mine = jnp.where(owner % sharers == at, columns[:, at * width : (at + 1) * width], mine)
    return mine


def project_block(step, me_ref, tokens_ref, key_ref, value_ref, out_ref):
    heads, _, width = out_ref.shape
    size = width // 2
    owner = me_ref[0] ^ step
    rows = tokens_ref[...]
    keys = jnp.dot(rows, key_ref[...], preferred_element_type=jnp.float32)
    values = jnp.dot(rows, value_ref[...], preferred_element_type=jnp.float32)
    keys = owned(keys, owner, heads * size).astype(out_ref.dtype)
    values = owned(values, owner, heads * size).astype(out_ref.dtype)
    for head in range(heads):
        part = slice(head * size, (head + 1) * size)
        out_ref[head] = jnp.concatenate([keys[:, part], values[:, part]], axis=-1)


def project(me, step, rows, count, key_weight, value_weight, heads, size):
    width = rows.shape[1]
    tiles = 2 if count % 32 == 0 else 1
    tile = count // tiles
    columns = max(heads * size, LANES)
    sharers = columns // (heads * size)

    def weight_index(i, s):
        return (0, (s[0] ^ step) // sharers)

    return pl.pallas_call(
        functools.partial(project_block, step),
        grid_spec=pltpu.PrefetchScalarGridSpec(
            num_scalar_prefetch=1,
            grid=(tiles,),
            in_specs=[
                pl.BlockSpec((tile, width), lambda i, s: (i, 0)),
                pl.BlockSpec((width, columns), weight_index),
                pl.BlockSpec((width, columns), weight_index),
            ],
            out_specs=pl.BlockSpec((heads, tile, 2 * size), lambda i, s: (0, i, 0)),
        ),
        out_shape=jax.ShapeDtypeStruct((heads, count, 2 * size), rows.dtype),
        cost_estimate=pl.CostEstimate(
            flops=4 * count * width * columns,
            bytes_accessed=2 * (count * width + 2 * width * columns + 2 * count * columns),
            transcendentals=0,
        ),
        name="project",
    )(me, rows, key_weight, value_weight)


def place_block(parts, length, block_ref, *refs):
    out_ref, left = refs[-2:]
    me = lax.axis_index("sp")
    writes = []
    for step, there, here, count in parts:
        start = pl.multiple_of((me ^ step) * length + there, ROWS)
        taken, put = block_ref.at[:, pl.ds(here, count), :], out_ref.at[:, pl.ds(start, count), :]
        writes.append(pltpu.make_async_copy(taken, put, left.at[len(writes)]))
    for write in writes:
        write.start()
    for write in writes:
        write.wait()


def place(cache, block, parts, places, length):
    heads, _, width = block.shape
    anywhere = pl.BlockSpec(memory_space=pl.ANY)
    old = () if cache is None else (cache,)
    return pl.pallas_call(
        functools.partial(place_block, parts, length),
        in_specs=[pl.BlockSpec(memory_space=pltpu.VMEM)] + [anywhere] * len(old),
        out_specs=anywhere,
        out_shape=jax.ShapeDtypeStruct((heads, places * length, width), block.dtype),
        scratch_shapes=[pltpu.SemaphoreType.DMA((len(parts),))],
        input_output_aliases={1: 0} if old else {},
        cost_estimate=pl.CostEstimate(flops=block.size, bytes_accessed=4 * block.size, transcendentals=0),
        compiler_params=pltpu.CompilerParams(vmem_limit_bytes=4 * MIB),
        name="place",
    )(block, *old)


def read_blocks(steps, near, me_ref, query_ref, gates_ref, borrowed_ref, *refs):
    block_refs, out_ref = refs[:-1], refs[-1]
    heads, _, width = block_refs[0].shape
    size = width // 2
    lanes = lax.broadcasted_iota(jnp.int32, (1, width), 1)
    for step, block_ref in zip(steps, block_refs):
        owner = me_ref[0] ^ step
        rows = block_ref.shape[1]
        for head in range(heads):
            block = block_ref[head]
            query = jnp.broadcast_to(query_ref[owner, pl.ds(head, 1), :], (8, width)).astype(block.dtype)
            scores = lax.dot_general(query, block, (((1,), (1,)), ((), ())), preferred_element_type=jnp.float32)
            gates = gates_ref[owner, pl.ds(head, 1), :]
            if step < near:
                more = borrowed_ref[lax.rem(owner, near), pl.ds(head, 1), :]
                gates = jnp.concatenate([gates, more], axis=-1)
            scores = scores[0:1] * size ** (-0.5) - gates[:, :rows]
            top = jnp.max(scores, axis=-1, keepdims=True)
            weights = jnp.exp(scores - top)
            total = jnp.sum(weights, axis=-1, keepdims=True)
            probs = jnp.broadcast_to(weights, (8, rows)).astype(block.dtype)
            weighted = jnp.dot(probs, block, preferred_element_type=jnp.float32)[0:1]
            row = jnp.where(lanes == 0, top, jnp.where(lanes == 1, total, weighted))
            out_ref[owner, pl.ds(head, 1), :] = row


def partial_reads(me, steps, near, queries, gates, borrowed, blocks):
    places, heads, size = queries.shape
    rows = gates.shape[2]
    queries = jnp.pad(queries.astype(jnp.float32), ((0, 0), (0, 0), (0, size)))
    whole = pl.BlockSpec(memory_space=pltpu.VMEM)
    return pl.pallas_call(
        functools.partial(read_blocks, steps, near),
        in_specs=[pl.BlockSpec(memory_space=pltpu.SMEM)] + [whole] * (3 + len(blocks)),
        out_specs=whole,
        out_shape=jax.ShapeDtypeStruct((places, heads, 2 * size), jnp.float32),
        cost_estimate=pl.CostEstimate(
            flops=16 * places * heads * rows * 2 * size,
            bytes_accessed=2 * places * heads * rows * 2 * size,
            transcendentals=places * heads * rows,
        ),
        name="read",
    )(me, queries, gates, borrowed, *blocks)


def merged_reads(parts, size):
    tops = parts[:, :, 0:1]
    top = jnp.max(tops, axis=0, keepdims=True)
    scale = jnp.exp(tops - top)
    total = jnp.sum(parts[:, :, 1:2] * scale, axis=0)
    weighted = jnp.sum(parts[:, :, size:] * scale, axis=0)
    return weighted / total


def packed_gates(gates):
    places, heads, length = gates.shape
    groups = gates.reshape(places, heads, length // LANES, LANES)
    first = groups[..., :1]
    falls = (groups - first).astype(jnp.bfloat16).reshape(gates.shape)
    rest, terms = first[..., 0], []
    for _ in range(3):
        terms.append(lax.reduce_precision(rest, 8, 7))
        rest = rest - terms[-1]
    return jnp.concatenate([falls] + [term.astype(jnp.bfloat16) for term in terms], axis=-1)


def unpacked_gates(packed, length):
    places, heads, _ = packed.shape
    packed = packed.astype(jnp.float32)
    falls, terms = packed[..., :length], packed[..., length:]
    first = jnp.sum(terms.reshape(places, heads, 3, length // LANES), axis=2)
    groups = falls.reshape(places, heads, length // LANES, LANES) + first[..., None]
    return groups.reshape(places, heads, length)


def plan(places):
    far = places // 2
    across = [places - 1] + list(range(far, places - 1))
    near = [far // 2] + [step for step in range(1, far) if step != far // 2]
    half = len(across) // 2
    order = across[:half] + near + across[half:]
    return order[:-1], order[-1:]


def on_device(places, tokens, key_weight, value_weight, cum_gate, query):
    heads, size = query.shape[1:]
    rows = tokens[0, 0]
    length = rows.shape[0]
    far = places // 2
    peer = far + far // 2
    me = lax.axis_index("sp").astype(jnp.int32)
    here = me.reshape(1)
    early, late = plan(places)
    kept = length - ROWS

    def swap(value, step):
        return lax.ppermute(value, "sp", [(i, i ^ step) for i in range(places)])

    def exchange(value):
        return lax.all_to_all(value, "sp", split_axis=0, concat_axis=0, tiled=True)

    lent = swap(rows[kept:], peer)
    more = jnp.concatenate([rows, lent], axis=0)

    def block_of(step):
        mine, count = (more, length + ROWS) if step < far else (rows, kept)
        return project(here, step, mine, count, key_weight, value_weight, heads, size)

    def parts_of(step):
        if step < far:
            return ((step, 0, 0, length), (step ^ peer, kept, length, ROWS))
        return ((step, 0, 0, kept),)

    sent, arrived = {}, []
    for step in early + late:
        sent[step] = block_of(step)
        pieces = [("", sent[step], parts_of(step))]
        if step in late:
            head = kept - TAIL
            pieces = [
                ("", sent[step][:, :head], ((step, 0, 0, head),)),
                ("_tail", sent[step][:, head:], ((step, head, 0, TAIL),)),
            ]
        for name, block, parts in pieces:
            arrived.append((f"place_{step}{name}", swap(block, step), parts))

    gates = cum_gate[0, :, 0, :].reshape(places, heads, length)
    asked = jnp.broadcast_to(query, (places, heads, size))
    told = exchange(jnp.concatenate([packed_gates(gates), asked], axis=-1))
    queries = told[:, :, -size:]
    gate_parts = unpacked_gates(told[:, :, :-size], length)
    gate_cache = jnp.transpose(gate_parts, (1, 0, 2)).reshape(1, heads, places * length)
    borrowed = lax.dynamic_slice(gates, ((me ^ far) & far, 0, kept), (far, heads, ROWS))
    borrowed = swap(borrowed.reshape(-1, LANES), peer).reshape(borrowed.shape)

    sent[0] = block_of(0)
    cache = place(None, sent[0], parts_of(0), places, length)
    steps = [0] + early + late
    parts = partial_reads(here, steps, far, queries, gates, borrowed, [sent[step] for step in steps])
    parts = exchange(parts)
    parts = lax.all_gather(parts, "tp", tiled=True)
    read = merged_reads(parts, size).astype(jnp.bfloat16)[None]

    for name, block, parts in arrived:
        if name == f"place_{late[-1]}":
            cache, read = lax.optimization_barrier((cache, read))
        cache = place(cache, block, parts, places, length)
    return (cache[None], gate_cache, read)


def solution(mesh):
    placed = (P("gr", "tp", "sp", None), P(), P(), P("gr", None, "tp", "sp"), P("gr", "sp", None))
    places = mesh.shape["sp"]

    def body(*args):
        return on_device(places, *args)

    return jax.shard_map(
        body,
        mesh=mesh,
        in_specs=placed,
        out_specs=(P("gr", "sp", "tp", None), P("gr", "sp", "tp"), P("gr", "sp", None)),
        check_vma=False,
    )
```
